32 devices in a mesh: kv: 4 (over y, x), tp: 8 (over z, core).
Axes of the slice: x: 2, y: 2, z: 4, core: 2. Of those that a mesh axis runs over, the one named last changes fastest.
Arguments:
- tokens: bfloat16 [128, 4096], P(None, ('kv', 'tp')), may hold values from -41 to 41
- lengths: int32 [128], P('kv'), may hold values from 1 to 8192, 262144 in all
- retention_state: float32 [128, 16, 128, 256], P('kv', 'tp'), may hold values from -4 to 4
- mixer_gain: float32 [4096], P('kv'), may hold values from 0.1 to 1.9
- query_weight: bfloat16 [4096, 2048], P('kv', 'tp'), may hold values from -0.09375 to 0.09375
- key_weight: bfloat16 [4096, 2048], P('kv', 'tp'), may hold values from -0.09375 to 0.09375
- value_weight: bfloat16 [4096, 4096], P('kv', 'tp'), may hold values from -0.09375 to 0.09375
- gate_weight: bfloat16 [4096, 4096], P('kv', 'tp'), may hold values from -0.09375 to 0.09375
- output_weight: bfloat16 [4096, 4096], P('tp', 'kv'), may hold values from -0.125 to 0.125
- channel_gain: float32 [4096], P('kv'), may hold values from 0.1 to 1.9
- ffn_gate: bfloat16 [4096, 11264], P('kv', 'tp'), may hold values from -0.09375 to 0.09375
- ffn_up: bfloat16 [4096, 11264], P('kv', 'tp'), may hold values from -0.09375 to 0.09375
- ffn_down: bfloat16 [11264, 4096], P('tp', 'kv'), may hold values from -0.078125 to 0.078125
Outputs:
- layer_output: bfloat16 [128, 4096], P(None, ('kv', 'tp'))
- new_state: float32 [128, 16, 128, 256], P('kv', 'tp')
The draws below stay inside these ranges and needn't reach their ends.
All inputs are finite; a program needn't handle non-finite values. No bound on the sum of `lengths` on one device may be relied on, other than what follows from the above.
Results may differ from the reference program's by a relative error of at most 0.022.
Values may be sent and summed in bfloat16 or wider, within the bound.
A program may use at most 64 MiB of HBM per device.

```python
import math
import jax
import jax.numpy as jnp
import numpy as np
from jax import lax

BATCH = 128
D = 4096
HEADS = 16
QK = 128
VD = 256
FF = 11264
MAXLEN = 8192


def draw_tokens(key, part):
    subkeys = jax.random.split(key, 3)
    positions = jnp.arange(D, dtype=jnp.float32) / (D - 1)
    roughness = jnp.exp(jax.random.uniform(subkeys[0], (D,), minval=-0.3, maxval=0.3))
    column_scale = jnp.exp(jnp.log(0.3) + positions * jnp.log(10.0)) * roughness
    base_values = jnp.clip(jax.random.normal(subkeys[2], (BATCH, D)), -5.0, 5.0)
    row_scale = jnp.exp(jax.random.uniform(subkeys[1], (BATCH, 1), minval=jnp.log(0.5), maxval=jnp.log(2.0)))
    return (base_values * row_scale * column_scale[None, :]).astype(jnp.bfloat16)


def with_spikes(entries, stream_key, source, target, parts, factor):
    def block_of(position):
        return (jnp.arange(entries.shape[position]) // (entries.shape[position] // parts)).reshape((-1,) + (1,) * (entries.ndim - 1 - position))

    near = jax.random.permutation(stream_key, parts)[block_of(target)]
    other_side = (block_of(target) + parts // 2) % parts
    return jnp.where((block_of(source) == near) | (block_of(source) == other_side), factor * entries, entries)


def levels(own_key, extent, cuts, low, largest):
    level, own = 1.0, jax.random.fold_in(own_key, 6)
    for dim, shards_of in cuts:
        steps = jnp.exp(jax.random.uniform(jax.random.fold_in(own, dim), (shards_of,), jnp.float32, low / len(cuts), largest / len(cuts)))
        level = level * jnp.repeat(steps, extent[dim] // shards_of).reshape([-1 if axis == dim else 1 for axis in range(len(extent))])
    return level


def split_up(count, total, bound, skew):
    weights = [(1 << 20) // math.isqrt(grade ** skew) + 1 for grade in range(2, count + 1)]
    spare, holding = total - bound - (count - 1), [1] * (count - 1)
    while spare > 0:
        movable = [i for i in range(count - 1) if holding[i] < bound]
        mass, left = sum([weights[i] for i in movable]), spare
        for i in movable:
            more = min(bound - holding[i], max(1, left * weights[i] // mass), spare)
            holding[i] = holding[i] + more
            spare = spare - more
    return np.array([bound] + holding)


def uneven_parts(rng, number_of, total, limit, skew):
    if number_of == 2:
        one = jax.random.randint(rng, (), max(1, total - limit), min(limit, total - 1) + 1)
        return jnp.stack([one, total - one])
    tallies = jnp.asarray(split_up(number_of, total, limit, skew), jnp.int32)
    couples = (number_of - 1) // 2
    source_of, receiver = tallies[1:1 + 2 * couples:2], tallies[2:2 + 2 * couples:2]
    margin = jnp.minimum(source_of - 1, limit - receiver)
    moved = jax.random.randint(jax.random.fold_in(rng, 1), (couples,), 0, 1 << 20) % (margin + 1)
    tallies = tallies.at[1:1 + 2 * couples:2].set(source_of - moved).at[2:2 + 2 * couples:2].set(receiver + moved)
    return tallies[jax.random.permutation(jax.random.fold_in(rng, 2), number_of)]


def centred(rng, extent, width, bound, cuts=(), kind=jnp.bfloat16):
    values = jax.random.normal(rng, extent, jnp.float32) * width
    if len(cuts) > 0:
        values = levels(rng, extent, cuts, -0.22, 0.18) * values
    return jnp.clip(values, min=-bound, max=bound).astype(kind)


def bell_draw_with(stream_key, shape, spread, limit, cuts, heavy, kind=jnp.bfloat16):
    drawn = spread * jax.random.normal(stream_key, shape, jnp.float32)
    if cuts:
        drawn = drawn * levels(stream_key, shape, cuts, -0.22, 0.18)
    return jnp.clip(with_spikes(drawn, jax.random.fold_in(stream_key, 3), *heavy), -limit, limit).astype(kind)


def setup_inputs(seed: int = 0) -> dict:
    streams_of = jax.random.split(jax.random.key(seed), 14)
    return {
        "tokens": draw_tokens(jax.random.fold_in(streams_of[13], 71), 0),
        "lengths": uneven_parts(streams_of[1], BATCH, BATCH * MAXLEN // 4, MAXLEN, 2).astype(jnp.int32),
        "retention_state": centred(streams_of[2], (BATCH, HEADS, QK, VD), 0.3, 4.0, ((0, 4), (1, 8)), jnp.float32),
        "mixer_gain": jnp.clip(1.0 + 0.18 * jax.random.normal(streams_of[3], (D,), jnp.float32), 0.1, 1.9),
        "query_weight": centred(streams_of[4], (D, HEADS * QK), D ** -0.5, 0.09375, ((0, 4), (1, 8))),
        "key_weight": centred(streams_of[5], (D, HEADS * QK), D ** -0.5, 0.09375, ((0, 4), (1, 8))),
        "value_weight": centred(streams_of[6], (D, HEADS * VD), D ** -0.5, 0.09375, ((0, 4), (1, 8))),
        "gate_weight": centred(streams_of[7], (D, HEADS * VD), D ** -0.5, 0.09375, ((0, 4), (1, 8))),
        "output_weight": bell_draw_with(streams_of[8], (HEADS * VD, D), D ** -0.5, 0.125, ((0, 8), (1, 4)), (0, 1, 8, 2.0)),
        "channel_gain": jnp.clip(1.0 + 0.18 * jax.random.normal(streams_of[9], (D,), jnp.float32), 0.1, 1.9),
        "ffn_gate": centred(streams_of[10], (D, FF), D ** -0.5, 0.09375, ((0, 4), (1, 8))),
        "ffn_up": centred(streams_of[11], (D, FF), D ** -0.5, 0.09375, ((0, 4), (1, 8))),
        "ffn_down": bell_draw_with(streams_of[12], (FF, D), FF ** -0.5, 0.078125, ((0, 8), (1, 4)), (0, 1, 8, 2.0)),
    }


def rotate_heads(vectors, positions):
    half_dim = vectors.shape[-1] // 2
    frequency = 10000.0 ** (-jnp.arange(half_dim, dtype=jnp.float32) / half_dim)
    angles = positions.astype(jnp.float32)[:, None, None] * frequency
    cosine = jnp.cos(angles)
    sine_part = jnp.sin(angles)
    first_half = vectors[..., :half_dim]
    second = vectors[..., half_dim:]
    return jnp.concatenate([first_half * cosine - second * sine_part, first_half * sine_part + second * cosine], axis=-1)

def inverse_rms(values):
    return lax.rsqrt(lax.optimization_barrier(jnp.mean(values * values, axis=-1)) + 1e-06)

def reference(tokens, lengths, retention_state, mixer_gain, query_weight, key_weight, value_weight, gate_weight, output_weight, channel_gain, ffn_gate, ffn_up, ffn_down):
    batch_rows = tokens.shape[0]
    tokens_wide = tokens.astype(jnp.float32)
    scale_one = inverse_rms(tokens_wide)[:, None]
    normed = (tokens_wide * mixer_gain).astype(jnp.bfloat16)
    query_proj = jnp.dot(normed, query_weight, preferred_element_type=jnp.float32) * scale_one
    query_rows = rotate_heads(query_proj.reshape(batch_rows, HEADS, QK), lengths).astype(jnp.bfloat16)
    key_proj = jnp.dot(normed, key_weight, preferred_element_type=jnp.float32) * scale_one
    key_rows = (rotate_heads(key_proj.reshape(batch_rows, HEADS, QK), lengths) * QK ** (-0.5)).astype(jnp.bfloat16)
    value_rows = (jnp.dot(normed, value_weight, preferred_element_type=jnp.float32) * scale_one).astype(jnp.bfloat16)
    value_rows = value_rows.reshape(batch_rows, HEADS, VD)
    gate_rows = jnp.dot(normed, gate_weight, preferred_element_type=jnp.float32) * scale_one
    head_ids = jnp.arange(HEADS, dtype=jnp.float32)
    decay_rate = 1.0 - 2.0 ** (-5.0 - 10.0 * head_ids / (HEADS - 1))
    new_state = decay_rate[None, :, None, None] * retention_state + key_rows.astype(jnp.float32)[..., :, None] * value_rows.astype(jnp.float32)[..., None, :]
    retained = jnp.einsum('bhk,bhkv->bhv', query_rows.astype(jnp.float32), new_state, precision=lax.Precision.HIGHEST)
    normalized = retained * inverse_rms(retained)[..., None]
    merged = (normalized.reshape(batch_rows, HEADS * VD) * jax.nn.silu(gate_rows)).astype(jnp.bfloat16)
    residual = (tokens_wide + jnp.dot(merged, output_weight, preferred_element_type=jnp.float32)).astype(jnp.bfloat16)
    residual_wide = residual.astype(jnp.float32)
    scale_two = inverse_rms(residual_wide)[:, None]
    normed_two = (residual_wide * channel_gain).astype(jnp.bfloat16)
    gate_ff = jnp.dot(normed_two, ffn_gate, preferred_element_type=jnp.float32) * scale_two
    up_ff = jnp.dot(normed_two, ffn_up, preferred_element_type=jnp.float32) * scale_two
    hidden = (jax.nn.silu(gate_ff) * up_ff).astype(jnp.bfloat16)
    layer_output = (residual_wide + jnp.dot(hidden, ffn_down, preferred_element_type=jnp.float32)).astype(jnp.bfloat16)
    return (layer_output, new_state)
```

```python
import functools

import jax
import jax.numpy as jnp
import numpy as np
from jax import lax
from jax.experimental import pallas as pl
from jax.experimental.pallas import tpu as pltpu
from jax.sharding import PartitionSpec as P

D = 4096
HEADS = 16
QK = 128
LANES = 128


def rotate_heads(vectors, positions):
    half_dim = vectors.shape[-1] // 2
    frequency = 10000.0 ** (-jnp.arange(half_dim, dtype=jnp.float32) / half_dim)
    angles = positions.astype(jnp.float32)[:, None, None] * frequency
    cosine = jnp.cos(angles)
    sine_part = jnp.sin(angles)
    first_half = vectors[..., :half_dim]
    second = vectors[..., half_dim:]
    return jnp.concatenate(
        [first_half * cosine - second * sine_part, first_half * sine_part + second * cosine],
        axis=-1,
    )


def gathered_rows(columns):
    return lax.all_gather(columns, "tp", axis=1, tiled=True)


def owned_sums(partial_value, squares):
    raw_sums, totals = (
        lax.psum_scatter(
            partial_value.astype(jnp.bfloat16), "kv", scatter_dimension=0, tiled=True
        ).astype(jnp.float32),
        lax.psum_scatter(
            squares.astype(jnp.bfloat16), "kv", scatter_dimension=0, tiled=True
        ).astype(jnp.float32),
    )
    summed = raw_sums * lax.rsqrt(totals / D + 1e-06)[:, None]
    return summed


def every_sum(partial_value, squares):
    raw_sums, totals = (
        lax.psum(partial_value.astype(jnp.bfloat16), "kv").astype(jnp.float32),
        lax.psum(squares.astype(jnp.bfloat16), "kv").astype(jnp.float32),
    )
    summed = raw_sums * lax.rsqrt(totals / D + 1e-06)[:, None]
    return summed


def on_device(
    tokens,
    lengths,
    retention_state,
    mixer_gain,
    query_weight,
    key_weight,
    value_weight,
    gate_weight,
    output_weight,
    channel_gain,
    ffn_gate,
    ffn_up,
    ffn_down,
):
    feature_block = gathered_rows(tokens).astype(jnp.float32)
    squares = jnp.sum(feature_block * feature_block, axis=1)
    normed = (feature_block * mixer_gain).astype(jnp.bfloat16)
    partial_value = jnp.concatenate(
        [
            jnp.dot(normed, query_weight, preferred_element_type=jnp.float32),
            jnp.dot(normed, key_weight, preferred_element_type=jnp.float32),
            jnp.dot(normed, value_weight, preferred_element_type=jnp.float32),
            jnp.dot(normed, gate_weight, preferred_element_type=jnp.float32),
        ],
        axis=1,
    )
    owned_rows = owned_sums(partial_value, squares)
    local_heads = query_weight.shape[1] // QK
    q_width = query_weight.shape[1]
    v_width = value_weight.shape[1]
    head_width = v_width // local_heads
    seq_rows = owned_rows.shape[0]
    query_rows = rotate_heads(
        owned_rows[:, :q_width].reshape(seq_rows, local_heads, QK), lengths
    ).astype(jnp.bfloat16)
    key_rows = (
        rotate_heads(
            owned_rows[:, q_width : 2 * q_width].reshape(seq_rows, local_heads, QK), lengths
        )
        * QK ** (-0.5)
    ).astype(jnp.bfloat16)
    value_rows = (
        owned_rows[:, 2 * q_width : 2 * q_width + v_width]
        .astype(jnp.bfloat16)
        .reshape(seq_rows, local_heads, head_width)
    )
    gate_rows = owned_rows[:, 2 * q_width + v_width :]
    head_ids = (lax.axis_index("tp") * local_heads + jnp.arange(local_heads)).astype(jnp.float32)
    decay_rate = 1.0 - 2.0 ** (-5.0 - 10.0 * head_ids / (HEADS - 1))
    new_state = (
        decay_rate[None, :, None, None] * retention_state
        + key_rows.astype(jnp.float32)[..., :, None] * value_rows.astype(jnp.float32)[..., None, :]
    )
    retained = jnp.einsum(
        "bhk,bhkv->bhv", query_rows.astype(jnp.float32), new_state, precision=lax.Precision.HIGHEST
    )
    normalized = retained * lax.rsqrt(jnp.mean(retained * retained, axis=-1) + 1e-06)[..., None]
    merged = (normalized.reshape(seq_rows, v_width) * jax.nn.silu(gate_rows)).astype(jnp.bfloat16)
    mixed_part = jnp.dot(
        lax.all_gather(merged, "kv", axis=0, tiled=True),
        output_weight,
        preferred_element_type=jnp.float32,
    )
    mixed_cols = lax.psum_scatter(
        mixed_part.astype(jnp.bfloat16), "tp", scatter_dimension=1, tiled=True
    ).astype(jnp.float32)
    residual = (tokens.astype(jnp.float32) + mixed_cols).astype(jnp.bfloat16)
    block_two = gathered_rows(residual).astype(jnp.float32)
    squares_two = jnp.sum(block_two * block_two, axis=1)
    normed_two = (block_two * channel_gain).astype(jnp.bfloat16)
    partial_two = jnp.concatenate(
        [
            jnp.dot(normed_two, ffn_gate, preferred_element_type=jnp.float32),
            jnp.dot(normed_two, ffn_up, preferred_element_type=jnp.float32),
        ],
        axis=1,
    )
    hidden_units = ffn_gate.shape[1]
    summed = every_sum(partial_two, squares_two)
    hidden = (jax.nn.silu(summed[:, :hidden_units]) * summed[:, hidden_units:]).astype(jnp.bfloat16)
    down_part = jnp.dot(hidden, ffn_down, preferred_element_type=jnp.float32)
    down_sums = lax.psum_scatter(
        down_part.astype(jnp.bfloat16), "tp", scatter_dimension=1, tiled=True
    ).astype(jnp.float32)
    layer_output = (residual.astype(jnp.float32) + down_sums).astype(jnp.bfloat16)
    return (layer_output, new_state)


MESH_ID = pl.DeviceIdType.MESH
VMEM_LIMIT = 48 * 1024 * 1024


def greet(axes):
    barrier = pltpu.get_barrier_semaphore()
    for axis, count, me in axes:
        for step in range(1, count):
            pl.semaphore_signal(
                barrier, inc=1, device_id={axis: lax.rem(me + step, count)}, device_id_type=MESH_ID
            )
    pl.semaphore_wait(barrier, sum(count - 1 for _, count, _ in axes))


def send_all(axis, count, me, source, target, send_sems, recv_sems):
    copies = []
    for step in range(1, count):
        peer = lax.rem(me + step, count)
        copy = pltpu.make_async_remote_copy(
            src_ref=source(peer),
            dst_ref=target(step),
            send_sem=send_sems.at[step - 1],
            recv_sem=recv_sems.at[step - 1],
            device_id={axis: peer},
            device_id_type=MESH_ID,
        )
        copy.start()
        copies.append(copy)
    return copies


def received(copies):
    for copy in copies:
        copy.wait_recv()


def sent(copies):
    for copy in copies:
        copy.wait_send()


def load_all(pairs, sems):
    copies = [pltpu.make_async_copy(src, dst, sems.at[i]) for i, (src, dst) in enumerate(pairs)]
    for copy in copies:
        copy.start()
    return copies


def silu(value):
    return value / (1.0 + jnp.exp(-value))


def square_block(squares):
    head = squares.astype(jnp.bfloat16).astype(jnp.float32)
    rest = squares - head
    lane = lax.broadcasted_iota(jnp.int32, (squares.shape[0], LANES), 1)
    return jnp.where(lane < LANES // 2, head, rest).astype(jnp.bfloat16)


def square_total(block):
    return block[:, :1] + block[:, LANES // 2 : LANES // 2 + 1]


def wide(ref):
    return jnp.concatenate([ref[j] for j in range(ref.shape[0])], axis=1)


def project_kernel(
    n_kv, n_tp, features,
    tokens, lengths, freq, gain, wq_hbm, wk_hbm, wv_hbm, wg_hbm,
    qk_out, v_out, gate_out,
    wq, wk, wv, wg, gathered, out_a, out_b, in_a, in_b,
    load_sems, gs, gr, as_, ar, bs, br,
):
    kv, tp = lax.axis_index("kv"), lax.axis_index("tp")
    loads = load_all([(wq_hbm, wq), (wk_hbm, wk), (wv_hbm, wv), (wg_hbm, wg)], load_sems)
    greet([("tp", n_tp, tp), ("kv", n_kv, kv)])
    copies = send_all("tp", n_tp, tp, lambda p: tokens, lambda s: gathered.at[tp], gs, gr)
    gathered[tp] = tokens[...]
    rows = out_a.shape[1]
    row = lax.broadcasted_iota(jnp.int32, (rows, rows), 0)
    col = lax.broadcasted_iota(jnp.int32, (rows, rows), 1)
    spread = jnp.where(row == col, lengths[...].astype(jnp.float32), 0.0)
    angles = jnp.sum(spread, axis=1, keepdims=True) * freq[...]
    cosine, sine = jnp.cos(angles), jnp.sin(angles)
    lane = lax.broadcasted_iota(jnp.int32, angles.shape, 1)
    sine = jnp.where(lane < QK // 2, -sine, sine)
    received(copies)
    x = wide(gathered).astype(jnp.float32)
    squares = jnp.sum(x * x, axis=1, keepdims=True)
    normed = (x * gain[...]).astype(jnp.bfloat16)
    q_width, v_width = wq.shape[1], wv.shape[1]

    def project(weight):
        full = jnp.dot(normed, weight[...], preferred_element_type=jnp.float32)
        return full.astype(jnp.bfloat16).reshape(n_kv, rows, full.shape[1])

    out_a[:, :, 2 * q_width :] = square_block(squares).reshape(n_kv, rows, LANES)
    loads[0].wait()
    out_a[:, :, :q_width] = project(wq)
    loads[1].wait()
    out_a[:, :, q_width : 2 * q_width] = project(wk)
    first = send_all("kv", n_kv, kv, lambda p: out_a.at[p], lambda s: in_a.at[s - 1], as_, ar)
    loads[2].wait()
    out_b[:, :, :v_width] = project(wv)
    loads[3].wait()
    out_b[:, :, v_width:] = project(wg)
    second = send_all("kv", n_kv, kv, lambda p: out_b.at[p], lambda s: in_b.at[s - 1], bs, br)
    received(first)
    total = out_a[kv].astype(jnp.float32)
    for step in range(n_kv - 1):
        total += in_a[step].astype(jnp.float32)
    scale = lax.rsqrt(square_total(total[:, 2 * q_width :]) / features + 1e-06)
    total = total * scale
    blocks = []
    for head in range(q_width // QK):
        for base, factor in ((0, 1.0), (q_width, QK ** (-0.5))):
            part = total[:, base + head * QK : base + (head + 1) * QK]
            turned = (part * cosine + pltpu.roll(part, QK // 2, 1) * sine) * factor
            blocks.append(turned.astype(jnp.bfloat16).astype(jnp.float32))
    qk_out[...] = jnp.concatenate(blocks, axis=0).T
    received(second)
    total = out_b[kv].astype(jnp.float32)
    for step in range(n_kv - 1):
        total += in_b[step].astype(jnp.float32)
    total = total * scale
    v_out[...] = total[:, :v_width].astype(jnp.bfloat16).astype(jnp.float32)
    gate_out[...] = silu(total[:, v_width:])
    sent(copies)
    sent(first)
    sent(second)


def state_kernel(n_tp, rows, qk, v, state, new_state, retained):
    block, heads = state.shape[0], state.shape[1]
    width = state.shape[3]
    start = pl.program_id(0) * block
    tp = lax.axis_index("tp")
    turned = pltpu.roll(qk[...], lax.rem(LANES - start, LANES), 1)
    for head in range(heads):
        number = jnp.full((1, width), tp * heads + head, jnp.int32).astype(jnp.float32)
        decay = 1.0 - jnp.exp2(-5.0 - 10.0 * number / (heads * n_tp - 1))
        for s in range(block):
            lane = 2 * head * rows + s
            query = turned[:, lane : lane + 1]
            key = turned[:, lane + rows : lane + rows + 1]
            value = v[pl.ds(start + s, 1), head * width : (head + 1) * width]
            new = decay * state[s, head] + key * value
            new_state[s, head] = new
            retained[pl.ds(start + s, 1), head * width : (head + 1) * width] = jnp.sum(
                query * new, axis=0, keepdims=True
            )


def mix_kernel(
    n_kv, n_tp, features, heads,
    retained, gate, tokens, gain, wo_hbm, wg_hbm, wu_hbm, wd_hbm,
    out,
    wo, wg, wu, wd, merged, mixed_out, mixed_in, own, gathered,
    up_out, gate_out, up_in, gate_in, hidden, down_out, down_in,
    load_sems, ms, mr, xs, xr, cs, cr, as_, ar, bs, br, hs, hr, ds_, dr,
):
    kv, tp = lax.axis_index("kv"), lax.axis_index("tp")
    loads = load_all([(wo_hbm, wo), (wg_hbm, wg), (wu_hbm, wu), (wd_hbm, wd)], load_sems)
    rows = retained.shape[0]
    width = retained.shape[1] // heads
    parts = []
    for head in range(heads):
        part = retained[:, head * width : (head + 1) * width]
        parts.append(part * lax.rsqrt(jnp.mean(part * part, axis=1, keepdims=True) + 1e-06))
    merged[kv] = (jnp.concatenate(parts, axis=1) * gate[...]).astype(jnp.bfloat16)
    greet([("tp", n_tp, tp), ("kv", n_kv, kv)])
    copies_m = send_all("kv", n_kv, kv, lambda p: merged.at[kv], lambda s: merged.at[kv], ms, mr)
    loads[0].wait()
    received(copies_m)
    batch = n_kv * rows
    columns = tokens.shape[1]

    def summed(lhs, weight, buffer_out, buffer_in, send_sems, recv_sems):
        full = jnp.dot(lhs, weight[...], preferred_element_type=jnp.float32).astype(jnp.bfloat16)
        for j in range(n_tp):
            buffer_out[j] = full[:, j * columns : (j + 1) * columns]
        copies = send_all(
            "tp", n_tp, tp, lambda p: buffer_out.at[p], lambda s: buffer_in.at[s - 1], send_sems, recv_sems
        )
        received(copies)
        total = buffer_out[tp].astype(jnp.float32)
        for step in range(n_tp - 1):
            total += buffer_in[step].astype(jnp.float32)
        return total, copies

    total, copies_x = summed(merged[...].reshape(batch, -1), wo, mixed_out, mixed_in, xs, xr)
    residual = (tokens[...].astype(jnp.float32) + total).astype(jnp.bfloat16)
    own[...] = residual
    gathered[tp] = residual
    copies_c = send_all("tp", n_tp, tp, lambda p: own, lambda s: gathered.at[tp], cs, cr)
    received(copies_c)
    x = wide(gathered).astype(jnp.float32)
    squares = jnp.sum(x * x, axis=1, keepdims=True)
    normed = (x * gain[...]).astype(jnp.bfloat16)
    units = wg.shape[1]

    def project(weight):
        full = jnp.dot(normed, weight[...], preferred_element_type=jnp.float32)
        return full.astype(jnp.bfloat16).reshape(n_kv, rows, full.shape[1])

    gate_out[:, :, units:] = square_block(squares).reshape(n_kv, rows, LANES)
    loads[1].wait()
    gate_out[:, :, :units] = project(wg)
    copies_a = send_all("kv", n_kv, kv, lambda p: gate_out.at[p], lambda s: gate_in.at[s - 1], as_, ar)
    loads[2].wait()
    up_out[...] = project(wu)
    copies_b = send_all("kv", n_kv, kv, lambda p: up_out.at[p], lambda s: up_in.at[s - 1], bs, br)
    received(copies_a)
    total = gate_out[kv].astype(jnp.float32)
    for step in range(n_kv - 1):
        total += gate_in[step].astype(jnp.float32)
    scale = lax.rsqrt(square_total(total[:, units:]) / features + 1e-06)
    activated = silu(total[:, :units] * scale)
    received(copies_b)
    total = up_out[kv].astype(jnp.float32)
    for step in range(n_kv - 1):
        total += up_in[step].astype(jnp.float32)
    hidden[kv] = (activated * (total * scale)).astype(jnp.bfloat16)
    copies_h = send_all("kv", n_kv, kv, lambda p: hidden.at[kv], lambda s: hidden.at[kv], hs, hr)
    loads[3].wait()
    received(copies_h)
    total, copies_d = summed(hidden[...].reshape(batch, units), wd, down_out, down_in, ds_, dr)
    out[...] = (own[...].astype(jnp.float32) + total).astype(jnp.bfloat16)
    for copies in (copies_m, copies_x, copies_c, copies_a, copies_b, copies_h, copies_d):
        sent(copies)


def fused_on_device(n_kv, n_tp, *arrays):
    (
        tokens, lengths, state, mixer_gain, wq, wk, wv, wg, wo, channel_gain, fg, fu, fd,
    ) = arrays
    batch, columns = tokens.shape
    rows, heads, _, width = state.shape
    depth, q_width = wq.shape
    v_width, units = wv.shape[1], fg.shape[1]
    features = depth * n_kv
    bf16, f32 = jnp.bfloat16, jnp.float32
    vmem = pl.BlockSpec(memory_space=pltpu.VMEM)
    hbm = pl.BlockSpec(memory_space=pltpu.HBM)
    dma = pltpu.SemaphoreType.DMA
    tp_sems, kv_sems = [dma((n_tp - 1,))] * 2, [dma((n_kv - 1,))] * 2
    index = np.arange(QK) % (QK // 2)
    freq = jnp.asarray((10000.0 ** (-index / (QK // 2))).astype(np.float32))[None, :]
    a_width, b_width = 2 * q_width + LANES, 2 * v_width
    qk, value, gate = pl.pallas_call(
        functools.partial(project_kernel, n_kv, n_tp, features),
        out_shape=(
            jax.ShapeDtypeStruct((QK, LANES), f32),
            jax.ShapeDtypeStruct((rows, v_width), f32),
            jax.ShapeDtypeStruct((rows, v_width), f32),
        ),
        in_specs=[vmem] * 4 + [hbm] * 4,
        out_specs=(vmem,) * 3,
        scratch_shapes=[
            pltpu.VMEM(wq.shape, bf16),
            pltpu.VMEM(wk.shape, bf16),
            pltpu.VMEM(wv.shape, bf16),
            pltpu.VMEM(wg.shape, bf16),
            pltpu.VMEM((n_tp, batch, columns), bf16),
            pltpu.VMEM((n_kv, rows, a_width), bf16),
            pltpu.VMEM((n_kv, rows, b_width), bf16),
            pltpu.VMEM((n_kv - 1, rows, a_width), bf16),
            pltpu.VMEM((n_kv - 1, rows, b_width), bf16),
            dma((4,)),
        ]
        + tp_sems + kv_sems + kv_sems,
        compiler_params=pltpu.CompilerParams(
            collective_id=0, has_side_effects=True, vmem_limit_bytes=VMEM_LIMIT
        ),
        name="project",
    )(tokens, lengths[None, :], freq, mixer_gain[None, :], wq, wk, wv, wg)

    block = 4
    state_spec = pl.BlockSpec((block, heads, QK, width), lambda i: (i, 0, 0, 0))
    new_state, retained = pl.pallas_call(
        functools.partial(state_kernel, n_tp, rows),
        grid=(rows // block,),
        out_shape=(
            jax.ShapeDtypeStruct(state.shape, f32),
            jax.ShapeDtypeStruct((rows, v_width), f32),
        ),
        in_specs=[
            pl.BlockSpec((QK, LANES), lambda i: (0, 0)),
            pl.BlockSpec((rows, v_width), lambda i: (0, 0)),
            state_spec,
        ],
        out_specs=(state_spec, pl.BlockSpec((rows, v_width), lambda i: (0, 0))),
        compiler_params=pltpu.CompilerParams(vmem_limit_bytes=VMEM_LIMIT),
        name="state",
    )(qk, value, state)

    layer_output = pl.pallas_call(
        functools.partial(mix_kernel, n_kv, n_tp, features, heads),
        out_shape=jax.ShapeDtypeStruct(tokens.shape, bf16),
        in_specs=[vmem] * 4 + [hbm] * 4,
        out_specs=vmem,
        scratch_shapes=[
            pltpu.VMEM(wo.shape, bf16),
            pltpu.VMEM(fg.shape, bf16),
            pltpu.VMEM(fu.shape, bf16),
            pltpu.VMEM(fd.shape, bf16),
            pltpu.VMEM((n_kv, rows, v_width), bf16),
            pltpu.VMEM((n_tp, batch, columns), bf16),
            pltpu.VMEM((n_tp - 1, batch, columns), bf16),
            pltpu.VMEM((batch, columns), bf16),
            pltpu.VMEM((n_tp, batch, columns), bf16),
            pltpu.VMEM((n_kv, rows, units), bf16),
            pltpu.VMEM((n_kv, rows, units + LANES), bf16),
            pltpu.VMEM((n_kv - 1, rows, units), bf16),
            pltpu.VMEM((n_kv - 1, rows, units + LANES), bf16),
            pltpu.VMEM((n_kv, rows, units), bf16),
            pltpu.VMEM((n_tp, batch, columns), bf16),
            pltpu.VMEM((n_tp - 1, batch, columns), bf16),
            dma((4,)),
        ]
        + kv_sems + tp_sems + tp_sems + kv_sems + kv_sems + kv_sems + tp_sems,
        compiler_params=pltpu.CompilerParams(
            collective_id=1, has_side_effects=True, vmem_limit_bytes=VMEM_LIMIT
        ),
        name="mix",
    )(retained, gate, tokens, channel_gain[None, :], wo, fg, fu, fd)
    return layer_output, new_state


def fits(n_kv, n_tp, arrays):
    tokens, state, ffn_gate = arrays[0], arrays[2], arrays[10]
    rows, heads = state.shape[0], state.shape[1]
    return (
        tokens.shape[1] % LANES == 0
        and ffn_gate.shape[1] % LANES == 0
        and rows % 16 == 0
        and 2 * heads * rows == LANES
        and state.shape[2] == QK == LANES
        and state.shape[3] % LANES == 0
    )


def per_device(n_kv, n_tp, *arrays):
    if fits(n_kv, n_tp, arrays):
        return fused_on_device(n_kv, n_tp, *arrays)
    return on_device(*arrays)


def solution(mesh):
    in_specs = (
        P(None, ("kv", "tp")),
        P("kv"),
        P("kv", "tp", None, None),
        P("kv"),
        P("kv", "tp"),
        P("kv", "tp"),
        P("kv", "tp"),
        P("kv", "tp"),
        P("tp", "kv"),
        P("kv"),
        P("kv", "tp"),
        P("kv", "tp"),
        P("tp", "kv"),
    )
    out_specs = (P(None, ("kv", "tp")), P("kv", "tp", None, None))
    return jax.shard_map(
        functools.partial(per_device, mesh.shape["kv"], mesh.shape["tp"]),
        mesh=mesh, in_specs=in_specs, out_specs=out_specs, check_vma=False
    )
```

```python
import functools

import jax
import jax.numpy as jnp
import numpy as np
from jax import lax
from jax.experimental import pallas as pl
from jax.experimental.pallas import tpu as pltpu
from jax.sharding import PartitionSpec as P

D = 4096
HEADS = 16
QK = 128
LANES = 128


def rotate_heads(vectors, positions):
    half_dim = vectors.shape[-1] // 2
    frequency = 10000.0 ** (-jnp.arange(half_dim, dtype=jnp.float32) / half_dim)
    angles = positions.astype(jnp.float32)[:, None, None] * frequency
    cosine = jnp.cos(angles)
    sine_part = jnp.sin(angles)
    first_half = vectors[..., :half_dim]
    second = vectors[..., half_dim:]
    return jnp.concatenate(
        [first_half * cosine - second * sine_part, first_half * sine_part + second * cosine],
        axis=-1,
    )


def gathered_rows(columns):
    return lax.all_gather(columns, "tp", axis=1, tiled=True)


def owned_sums(partial_value, squares):
    raw_sums, totals = (
        lax.psum_scatter(
            partial_value.astype(jnp.bfloat16), "kv", scatter_dimension=0, tiled=True
        ).astype(jnp.float32),
        lax.psum_scatter(
            squares.astype(jnp.bfloat16), "kv", scatter_dimension=0, tiled=True
        ).astype(jnp.float32),
    )
    summed = raw_sums * lax.rsqrt(totals / D + 1e-06)[:, None]
    return summed


def every_sum(partial_value, squares):
    raw_sums, totals = (
        lax.psum(partial_value.astype(jnp.bfloat16), "kv").astype(jnp.float32),
        lax.psum(squares.astype(jnp.bfloat16), "kv").astype(jnp.float32),
    )
    summed = raw_sums * lax.rsqrt(totals / D + 1e-06)[:, None]
    return summed


def on_device(
    tokens,
    lengths,
    retention_state,
    mixer_gain,
    query_weight,
    key_weight,
    value_weight,
    gate_weight,
    output_weight,
    channel_gain,
    ffn_gate,
    ffn_up,
    ffn_down,
):
    feature_block = gathered_rows(tokens).astype(jnp.float32)
    squares = jnp.sum(feature_block * feature_block, axis=1)
    normed = (feature_block * mixer_gain).astype(jnp.bfloat16)
    partial_value = jnp.concatenate(
        [
            jnp.dot(normed, query_weight, preferred_element_type=jnp.float32),
            jnp.dot(normed, key_weight, preferred_element_type=jnp.float32),
            jnp.dot(normed, value_weight, preferred_element_type=jnp.float32),
            jnp.dot(normed, gate_weight, preferred_element_type=jnp.float32),
        ],
        axis=1,
    )
    owned_rows = owned_sums(partial_value, squares)
    local_heads = query_weight.shape[1] // QK
    q_width = query_weight.shape[1]
    v_width = value_weight.shape[1]
    head_width = v_width // local_heads
    seq_rows = owned_rows.shape[0]
    query_rows = rotate_heads(
        owned_rows[:, :q_width].reshape(seq_rows, local_heads, QK), lengths
    ).astype(jnp.bfloat16)
    key_rows = (
        rotate_heads(
            owned_rows[:, q_width : 2 * q_width].reshape(seq_rows, local_heads, QK), lengths
        )
        * QK ** (-0.5)
    ).astype(jnp.bfloat16)
    value_rows = (
        owned_rows[:, 2 * q_width : 2 * q_width + v_width]
        .astype(jnp.bfloat16)
        .reshape(seq_rows, local_heads, head_width)
    )
    gate_rows = owned_rows[:, 2 * q_width + v_width :]
    head_ids = (lax.axis_index("tp") * local_heads + jnp.arange(local_heads)).astype(jnp.float32)
    decay_rate = 1.0 - 2.0 ** (-5.0 - 10.0 * head_ids / (HEADS - 1))
    new_state = (
        decay_rate[None, :, None, None] * retention_state
        + key_rows.astype(jnp.float32)[..., :, None] * value_rows.astype(jnp.float32)[..., None, :]
    )
    retained = jnp.einsum(
        "bhk,bhkv->bhv", query_rows.astype(jnp.float32), new_state, precision=lax.Precision.HIGHEST
    )
    normalized = retained * lax.rsqrt(jnp.mean(retained * retained, axis=-1) + 1e-06)[..., None]
    merged = (normalized.reshape(seq_rows, v_width) * jax.nn.silu(gate_rows)).astype(jnp.bfloat16)
    mixed_part = jnp.dot(
        lax.all_gather(merged, "kv", axis=0, tiled=True),
        output_weight,
        preferred_element_type=jnp.float32,
    )
    mixed_cols = lax.psum_scatter(
        mixed_part.astype(jnp.bfloat16), "tp", scatter_dimension=1, tiled=True
    ).astype(jnp.float32)
    residual = (tokens.astype(jnp.float32) + mixed_cols).astype(jnp.bfloat16)
    block_two = gathered_rows(residual).astype(jnp.float32)
    squares_two = jnp.sum(block_two * block_two, axis=1)
    normed_two = (block_two * channel_gain).astype(jnp.bfloat16)
    partial_two = jnp.concatenate(
        [
            jnp.dot(normed_two, ffn_gate, preferred_element_type=jnp.float32),
            jnp.dot(normed_two, ffn_up, preferred_element_type=jnp.float32),
        ],
        axis=1,
    )
    hidden_units = ffn_gate.shape[1]
    summed = every_sum(partial_two, squares_two)
    hidden = (jax.nn.silu(summed[:, :hidden_units]) * summed[:, hidden_units:]).astype(jnp.bfloat16)
    down_part = jnp.dot(hidden, ffn_down, preferred_element_type=jnp.float32)
    down_sums = lax.psum_scatter(
        down_part.astype(jnp.bfloat16), "tp", scatter_dimension=1, tiled=True
    ).astype(jnp.float32)
    layer_output = (residual.astype(jnp.float32) + down_sums).astype(jnp.bfloat16)
    return (layer_output, new_state)


MESH_ID = pl.DeviceIdType.MESH
VMEM_TOTAL = 67043328
CORES = 2


def greet(groups):
    barrier = pltpu.get_barrier_semaphore()
    for axis, peers in groups:
        for peer in peers:
            pl.semaphore_signal(barrier, inc=1, device_id={axis: peer}, device_id_type=MESH_ID)
    pl.semaphore_wait(barrier, sum(len(peers) for _, peers in groups))


def send_all(axis, count, me, source, target, send_sems, recv_sems):
    copies = []
    for step in range(1, count):
        peer = lax.rem(me + step, count)
        copy = pltpu.make_async_remote_copy(
            src_ref=source(peer),
            dst_ref=target(step),
            send_sem=send_sems.at[step - 1],
            recv_sem=recv_sems.at[step - 1],
            device_id={axis: peer},
            device_id_type=MESH_ID,
        )
        copy.start()
        copies.append(copy)
    return copies


def received(copies):
    for copy in copies:
        copy.wait_recv()


def sent(copies):
    for copy in copies:
        copy.wait_send()


def load_all(pairs, sems):
    copies = [pltpu.make_async_copy(src, dst, sems.at[i]) for i, (src, dst) in enumerate(pairs)]
    for copy in copies:
        copy.start()
    return copies


def silu(value):
    return value / (1.0 + jnp.exp(-value))


def square_block(squares):
    head = squares.astype(jnp.bfloat16).astype(jnp.float32)
    rest = squares - head
    lane = lax.broadcasted_iota(jnp.int32, (squares.shape[0], LANES), 1)
    return jnp.where(lane < LANES // 2, head, rest).astype(jnp.bfloat16)


def square_total(block):
    return block[:, :1] + block[:, LANES // 2 : LANES // 2 + 1]


def wide(ref):
    return jnp.concatenate([ref[j] for j in range(ref.shape[0])], axis=1)


def remote(axis, peer, source, target, send_sem, recv_sem):
    return pltpu.make_async_remote_copy(
        src_ref=source, dst_ref=target, send_sem=send_sem, recv_sem=recv_sem,
        device_id={axis: peer}, device_id_type=MESH_ID,
    )


def gather_tp(slots, source, tp, n_tp, send_sems, recv_sems):
    chips = n_tp // CORES
    chip, core = tp // CORES, lax.rem(tp, CORES)
    partner = chip * CORES + 1 - core
    direct = []
    for step in range(1, chips):
        peer = lax.rem(chip + step, chips) * CORES + core
        direct.append(
            remote("tp", peer, source, slots.at[tp], send_sems.at[step], recv_sems.at[step])
        )
    across = [remote("tp", partner, source, slots.at[tp], send_sems.at[0], recv_sems.at[0])]
    for copy in direct + across:
        copy.start()

    def finish():
        for step in range(1, chips):
            direct[step - 1].wait_recv()
            slot = lax.rem(chip - step + chips, chips) * CORES + core
            i = chips - 1 + step
            copy = remote(
                "tp", partner, slots.at[slot], slots.at[slot], send_sems.at[i], recv_sems.at[i]
            )
            copy.start()
            across.append(copy)
        received(across)
        return direct + across

    return finish


def reduce_tp(lhs, weight, parts, swapped, staged, landed, tp, n_tp, send_sems, recv_sems):
    chips = n_tp // CORES
    chip, core = tp // CORES, lax.rem(tp, CORES)
    partner = chip * CORES + 1 - core
    columns = parts.shape[3]
    full = jnp.dot(lhs, weight[...], preferred_element_type=jnp.float32).astype(jnp.bfloat16)
    for j in range(n_tp):
        parts[j % CORES, j // CORES] = full[:, j * columns : (j + 1) * columns]
    swap = remote(
        "tp", partner, parts.at[1 - core], swapped, send_sems.at[0], recv_sems.at[0]
    )
    swap.start()
    swap.wait_recv()
    copies = []
    for step in range(1, chips):
        other = lax.rem(chip + step, chips)
        pair = parts[core, other].astype(jnp.float32) + swapped[other].astype(jnp.float32)
        staged[step - 1] = pair.astype(jnp.bfloat16)
        copy = remote(
            "tp", other * CORES + core, staged.at[step - 1], landed.at[step - 1],
            send_sems.at[step], recv_sems.at[step],
        )
        copy.start()
        copies.append(copy)
    total = parts[core, chip].astype(jnp.float32) + swapped[chip].astype(jnp.float32)
    for step in range(1, chips):
        copies[step - 1].wait_recv()
        total += landed[step - 1].astype(jnp.float32)
    return total, copies + [swap]


def total_of(own, landed):
    total = own.astype(jnp.float32)
    for step in range(landed.shape[0]):
        total += landed[step].astype(jnp.float32)
    return total


def layer_kernel(
    n_kv, n_tp, features,
    tokens_hbm, lengths_hbm, freq_hbm, gain_hbm, gain_two_hbm, state_hbm,
    wq_hbm, wk_hbm, wv_hbm, wg_hbm, wo_hbm, fg_hbm, fu_hbm, fd_hbm,
    out, state_out,
    state, lengths, freq, gain, gain_two, wq, wk, wv, wg, wo, fg, fu, fd,
    gathered, out_a, out_b, in_a, in_b, qk, value, retained, merged,
    parts_x, swapped_x, staged_x, landed_x, own, gathered_two,
    gate_out, up_out, gate_in, up_in, hidden, parts_d, swapped_d, staged_d, landed_d,
    load_sems, store_sem, gs, gr, as_, ar, bs, br, ms, mr, xs, xr, cs, cr, es, er, fs, fr, hs, hr, ds_, dr,
):
    kv, tp = lax.axis_index("kv"), lax.axis_index("tp")
    chips = n_tp // CORES
    chip, core = tp // CORES, lax.rem(tp, CORES)
    pairs = [
        (tokens_hbm, gathered.at[tp]), (lengths_hbm, lengths), (freq_hbm, freq), (gain_hbm, gain),
        (wq_hbm, wq), (wk_hbm, wk), (wv_hbm, wv), (wg_hbm, wg), (state_hbm, state),
        (gain_two_hbm, gain_two), (wo_hbm, wo), (fg_hbm, fg), (fu_hbm, fu), (fd_hbm, fd),
    ]
    loads = load_all(pairs, load_sems)
    along = [lax.rem(chip + step, chips) * CORES + core for step in range(1, chips)]
    greet([
        ("tp", along + [chip * CORES + 1 - core]),
        ("kv", [lax.rem(kv + step, n_kv) for step in range(1, n_kv)]),
    ])
    loads[0].wait()
    finish_g = gather_tp(gathered, gathered.at[tp], tp, n_tp, gs, gr)
    for i in (1, 2, 3):
        loads[i].wait()
    rows = out_a.shape[1]
    row = lax.broadcasted_iota(jnp.int32, (rows, rows), 0)
    col = lax.broadcasted_iota(jnp.int32, (rows, rows), 1)
    spread = jnp.where(row == col, lengths[...].astype(jnp.float32), 0.0)
    angles = jnp.sum(spread, axis=1, keepdims=True) * freq[...]
    cosine, sine = jnp.cos(angles), jnp.sin(angles)
    lane = lax.broadcasted_iota(jnp.int32, angles.shape, 1)
    sine = jnp.where(lane < QK // 2, -sine, sine)
    started = finish_g()

    def normalise(slots, gains):
        x = wide(slots).astype(jnp.float32)
        squares = jnp.sum(x * x, axis=1, keepdims=True)
        return (x * gains[...]).astype(jnp.bfloat16), square_block(squares).reshape(n_kv, rows, LANES)

    def project(lhs, weight):
        full = jnp.dot(lhs, weight[...], preferred_element_type=jnp.float32)
        return full.astype(jnp.bfloat16).reshape(n_kv, rows, full.shape[1])

    normed, squares = normalise(gathered, gain)
    q_width, v_width = wq.shape[1], wv.shape[1]
    heads = q_width // QK
    width = v_width // heads
    out_a[:, :, 2 * q_width :] = squares
    loads[4].wait()
    out_a[:, :, :q_width] = project(normed, wq)
    loads[5].wait()
    out_a[:, :, q_width : 2 * q_width] = project(normed, wk)
    first = send_all("kv", n_kv, kv, lambda p: out_a.at[p], lambda s: in_a.at[s - 1], as_, ar)
    loads[6].wait()
    out_b[:, :, :v_width] = project(normed, wv)
    loads[7].wait()
    out_b[:, :, v_width:] = project(normed, wg)
    second = send_all("kv", n_kv, kv, lambda p: out_b.at[p], lambda s: in_b.at[s - 1], bs, br)
    loads[8].wait()
    received(first)
    total = total_of(out_a[kv], in_a)
    scale = lax.rsqrt(square_total(total[:, 2 * q_width :]) / features + 1e-06)
    total = total * scale
    blocks = []
    for base, factor in ((0, 1.0), (q_width, QK ** (-0.5))):
        for head in range(heads):
            part = total[:, base + head * QK : base + (head + 1) * QK]
            turned = (part * cosine + pltpu.roll(part, QK // 2, 1) * sine) * factor
            blocks.append(turned.astype(jnp.bfloat16).astype(jnp.float32))
    qk[...] = jnp.concatenate(blocks, axis=0).T
    block = 4

    def turned_to(start):
        return pltpu.roll(qk[...], lax.rem(LANES - start, LANES), 1)

    def query_step(i, carry):
        start = i * block
        turned = turned_to(start)
        for s in range(block):
            for head in range(heads):
                query = turned[:, head * rows + s : head * rows + s + 1]
                retained[pl.ds(start + s, 1), head * width : (head + 1) * width] = jnp.sum(
                    query * state[start + s, head], axis=0, keepdims=True
                )
        return carry

    lax.fori_loop(0, rows // block, query_step, 0)
    decays = []
    for head in range(heads):
        number = jnp.full((1, width), tp * heads + head, jnp.int32).astype(jnp.float32)
        decays.append(1.0 - jnp.exp2(-5.0 - 10.0 * number / (heads * n_tp - 1)))
    received(second)
    total = total_of(out_b[kv], in_b) * scale
    value[...] = total[:, :v_width].astype(jnp.bfloat16).astype(jnp.float32)
    pieces = []
    for head in range(heads):
        overlap = jnp.sum(blocks[head] * blocks[heads + head], axis=1, keepdims=True)
        span = slice(head * width, (head + 1) * width)
        piece = decays[head] * retained[:, span] + overlap * value[:, span]
        pieces.append(piece * lax.rsqrt(jnp.mean(piece * piece, axis=1, keepdims=True) + 1e-06))
    merged[kv] = (jnp.concatenate(pieces, axis=1) * silu(total[:, v_width:])).astype(jnp.bfloat16)
    copies_m = send_all("kv", n_kv, kv, lambda p: merged.at[kv], lambda s: merged.at[kv], ms, mr)

    def update_step(i, carry):
        start = i * block
        turned = turned_to(start)
        for s in range(block):
            for head in range(heads):
                lane = (heads + head) * rows + s
                outer = turned[:, lane : lane + 1] * value[pl.ds(start + s, 1), head * width : (head + 1) * width]
                state[start + s, head] = decays[head] * state[start + s, head] + outer
        return carry

    lax.fori_loop(0, rows // block, update_step, 0)
    loads[10].wait()
    received(copies_m)
    store = pltpu.make_async_copy(state, state_out, store_sem)
    store.start()
    batch = n_kv * rows
    total, copies_x = reduce_tp(
        merged[...].reshape(batch, v_width), wo, parts_x, swapped_x, staged_x, landed_x, tp, n_tp, xs, xr
    )
    residual = (tokens_of(gathered, tp) + total).astype(jnp.bfloat16)
    own[...] = residual
    gathered_two[tp] = residual
    finish_c = gather_tp(gathered_two, own, tp, n_tp, cs, cr)
    loads[9].wait()
    loads[11].wait()
    copies_c = finish_c()
    normed, squares = normalise(gathered_two, gain_two)
    units = fg.shape[1]
    gate_out[:, :, units:] = squares
    gate_out[:, :, :units] = project(normed, fg)
    copies_e = send_all("kv", n_kv, kv, lambda p: gate_out.at[p], lambda s: gate_in.at[s - 1], es, er)
    loads[12].wait()
    up_out[...] = project(normed, fu)
    copies_f = send_all("kv", n_kv, kv, lambda p: up_out.at[p], lambda s: up_in.at[s - 1], fs, fr)
    received(copies_e)
    total = total_of(gate_out[kv], gate_in)
    scale = lax.rsqrt(square_total(total[:, units:]) / features + 1e-06)
    activated = silu(total[:, :units] * scale)
    received(copies_f)
    hidden[kv] = (activated * (total_of(up_out[kv], up_in) * scale)).astype(jnp.bfloat16)
    copies_h = send_all("kv", n_kv, kv, lambda p: hidden.at[kv], lambda s: hidden.at[kv], hs, hr)
    loads[13].wait()
    received(copies_h)
    total, copies_d = reduce_tp(
        hidden[...].reshape(batch, units), fd, parts_d, swapped_d, staged_d, landed_d, tp, n_tp, ds_, dr
    )
    out[...] = (own[...].astype(jnp.float32) + total).astype(jnp.bfloat16)
    for copies in (started, first, second, copies_m, copies_x, copies_c, copies_e, copies_f, copies_h, copies_d):
        sent(copies)
    store.wait()


def tokens_of(slots, tp):
    return slots[tp].astype(jnp.float32)


def fused_on_device(n_kv, n_tp, *arrays):
    (
        tokens, lengths, state, mixer_gain, wq, wk, wv, wg, wo, channel_gain, fg, fu, fd,
    ) = arrays
    batch, columns = tokens.shape
    rows = state.shape[0]
    depth, q_width = wq.shape
    v_width, units = wv.shape[1], fg.shape[1]
    bf16, f32 = jnp.bfloat16, jnp.float32
    vmem = pl.BlockSpec(memory_space=pltpu.VMEM)
    hbm = pl.BlockSpec(memory_space=pltpu.HBM)
    dma = pltpu.SemaphoreType.DMA
    tp_sems, kv_sems = [dma((n_tp - 1,))] * 2, [dma((n_kv - 1,))] * 2
    chips = n_tp // CORES
    chip_sems = [dma((chips,))] * 2
    index = np.arange(QK) % (QK // 2)
    freq = jnp.asarray((10000.0 ** (-index / (QK // 2))).astype(np.float32))[None, :]
    a_width, b_width = 2 * q_width + LANES, 2 * v_width
    reduce_scratch = [
        pltpu.VMEM((CORES, chips, batch, columns), bf16),
        pltpu.VMEM((chips, batch, columns), bf16),
        pltpu.VMEM((chips - 1, batch, columns), bf16),
        pltpu.VMEM((chips - 1, batch, columns), bf16),
    ]
    return pl.pallas_call(
        functools.partial(layer_kernel, n_kv, n_tp, depth * n_kv),
        out_shape=(
            jax.ShapeDtypeStruct(tokens.shape, bf16),
            jax.ShapeDtypeStruct(state.shape, f32),
        ),
        in_specs=[hbm] * 14,
        out_specs=(vmem, hbm),
        scratch_shapes=[
            pltpu.VMEM(state.shape, f32),
            pltpu.VMEM((1, rows), jnp.int32),
            pltpu.VMEM((1, QK), f32),
            pltpu.VMEM((1, depth), f32),
            pltpu.VMEM((1, depth), f32),
        ]
        + [pltpu.VMEM(w.shape, bf16) for w in (wq, wk, wv, wg, wo, fg, fu, fd)]
        + [
            pltpu.VMEM((n_tp, batch, columns), bf16),
            pltpu.VMEM((n_kv, rows, a_width), bf16),
            pltpu.VMEM((n_kv, rows, b_width), bf16),
            pltpu.VMEM((n_kv - 1, rows, a_width), bf16),
            pltpu.VMEM((n_kv - 1, rows, b_width), bf16),
            pltpu.VMEM((QK, LANES), f32),
            pltpu.VMEM((rows, v_width), f32),
            pltpu.VMEM((rows, v_width), f32),
            pltpu.VMEM((n_kv, rows, v_width), bf16),
        ]
        + reduce_scratch
        + [
            pltpu.VMEM((batch, columns), bf16),
            pltpu.VMEM((n_tp, batch, columns), bf16),
            pltpu.VMEM((n_kv, rows, units + LANES), bf16),
            pltpu.VMEM((n_kv, rows, units), bf16),
            pltpu.VMEM((n_kv - 1, rows, units + LANES), bf16),
            pltpu.VMEM((n_kv - 1, rows, units), bf16),
            pltpu.VMEM((n_kv, rows, units), bf16),
        ]
        + reduce_scratch
        + [dma((14,)), dma]
        + tp_sems + kv_sems + kv_sems + kv_sems + chip_sems + tp_sems + kv_sems + kv_sems + kv_sems + chip_sems,
        compiler_params=pltpu.CompilerParams(
            collective_id=0, has_side_effects=True, vmem_limit_bytes=VMEM_TOTAL
        ),
        name="layer",
    )(tokens, lengths[None, :], freq, mixer_gain[None, :], channel_gain[None, :], state, wq, wk, wv, wg, wo, fg, fu, fd)


def fits(n_kv, n_tp, arrays):
    tokens, state, ffn_gate = arrays[0], arrays[2], arrays[10]
    rows, heads = state.shape[0], state.shape[1]
    return (
        tokens.shape[1] % LANES == 0
        and n_tp % CORES == 0
        and n_tp > CORES
        and n_kv > 1
        and 4 * state.size < VMEM_TOTAL // 4
        and ffn_gate.shape[1] % LANES == 0
        and rows % 16 == 0
        and 2 * heads * rows == LANES
        and state.shape[2] == QK == LANES
        and state.shape[3] % LANES == 0
    )


def per_device(n_kv, n_tp, *arrays):
    if fits(n_kv, n_tp, arrays):
        return fused_on_device(n_kv, n_tp, *arrays)
    return on_device(*arrays)


def solution(mesh):
    in_specs = (
        P(None, ("kv", "tp")),
        P("kv"),
        P("kv", "tp", None, None),
        P("kv"),
        P("kv", "tp"),
        P("kv", "tp"),
        P("kv", "tp"),
        P("kv", "tp"),
        P("tp", "kv"),
        P("kv"),
        P("kv", "tp"),
        P("kv", "tp"),
        P("tp", "kv"),
    )
    out_specs = (P(None, ("kv", "tp")), P("kv", "tp", None, None))
    return jax.shard_map(
        functools.partial(per_device, mesh.shape["kv"], mesh.shape["tp"]),
        mesh=mesh, in_specs=in_specs, out_specs=out_specs, check_vma=False
    )
```

```python
import functools

import jax
import jax.numpy as jnp
import numpy as np
from jax import lax
from jax.experimental import pallas as pl
from jax.experimental.pallas import tpu as pltpu
from jax.sharding import PartitionSpec as P

D = 4096
HEADS = 16
QK = 128
LANES = 128


def rotate_heads(vectors, positions):
    half_dim = vectors.shape[-1] // 2
    frequency = 10000.0 ** (-jnp.arange(half_dim, dtype=jnp.float32) / half_dim)
    angles = positions.astype(jnp.float32)[:, None, None] * frequency
    cosine = jnp.cos(angles)
    sine_part = jnp.sin(angles)
    first_half = vectors[..., :half_dim]
    second = vectors[..., half_dim:]
    return jnp.concatenate(
        [first_half * cosine - second * sine_part, first_half * sine_part + second * cosine],
        axis=-1,
    )


def gathered_rows(columns):
    return lax.all_gather(columns, "tp", axis=1, tiled=True)


def owned_sums(partial_value, squares):
    raw_sums, totals = (
        lax.psum_scatter(
            partial_value.astype(jnp.bfloat16), "kv", scatter_dimension=0, tiled=True
        ).astype(jnp.float32),
        lax.psum_scatter(
            squares.astype(jnp.bfloat16), "kv", scatter_dimension=0, tiled=True
        ).astype(jnp.float32),
    )
    summed = raw_sums * lax.rsqrt(totals / D + 1e-06)[:, None]
    return summed


def every_sum(partial_value, squares):
    raw_sums, totals = (
        lax.psum(partial_value.astype(jnp.bfloat16), "kv").astype(jnp.float32),
        lax.psum(squares.astype(jnp.bfloat16), "kv").astype(jnp.float32),
    )
    summed = raw_sums * lax.rsqrt(totals / D + 1e-06)[:, None]
    return summed


def on_device(
    tokens,
    lengths,
    retention_state,
    mixer_gain,
    query_weight,
    key_weight,
    value_weight,
    gate_weight,
    output_weight,
    channel_gain,
    ffn_gate,
    ffn_up,
    ffn_down,
):
    feature_block = gathered_rows(tokens).astype(jnp.float32)
    squares = jnp.sum(feature_block * feature_block, axis=1)
    normed = (feature_block * mixer_gain).astype(jnp.bfloat16)
    partial_value = jnp.concatenate(
        [
            jnp.dot(normed, query_weight, preferred_element_type=jnp.float32),
            jnp.dot(normed, key_weight, preferred_element_type=jnp.float32),
            jnp.dot(normed, value_weight, preferred_element_type=jnp.float32),
            jnp.dot(normed, gate_weight, preferred_element_type=jnp.float32),
        ],
        axis=1,
    )
    owned_rows = owned_sums(partial_value, squares)
    local_heads = query_weight.shape[1] // QK
    q_width = query_weight.shape[1]
    v_width = value_weight.shape[1]
    head_width = v_width // local_heads
    seq_rows = owned_rows.shape[0]
    query_rows = rotate_heads(
        owned_rows[:, :q_width].reshape(seq_rows, local_heads, QK), lengths
    ).astype(jnp.bfloat16)
    key_rows = (
        rotate_heads(
            owned_rows[:, q_width : 2 * q_width].reshape(seq_rows, local_heads, QK), lengths
        )
        * QK ** (-0.5)
    ).astype(jnp.bfloat16)
    value_rows = (
        owned_rows[:, 2 * q_width : 2 * q_width + v_width]
        .astype(jnp.bfloat16)
        .reshape(seq_rows, local_heads, head_width)
    )
    gate_rows = owned_rows[:, 2 * q_width + v_width :]
    head_ids = (lax.axis_index("tp") * local_heads + jnp.arange(local_heads)).astype(jnp.float32)
    decay_rate = 1.0 - 2.0 ** (-5.0 - 10.0 * head_ids / (HEADS - 1))
    new_state = (
        decay_rate[None, :, None, None] * retention_state
        + key_rows.astype(jnp.float32)[..., :, None] * value_rows.astype(jnp.float32)[..., None, :]
    )
    retained = jnp.einsum(
        "bhk,bhkv->bhv", query_rows.astype(jnp.float32), new_state, precision=lax.Precision.HIGHEST
    )
    normalized = retained * lax.rsqrt(jnp.mean(retained * retained, axis=-1) + 1e-06)[..., None]
    merged = (normalized.reshape(seq_rows, v_width) * jax.nn.silu(gate_rows)).astype(jnp.bfloat16)
    mixed_part = jnp.dot(
        lax.all_gather(merged, "kv", axis=0, tiled=True),
        output_weight,
        preferred_element_type=jnp.float32,
    )
    mixed_cols = lax.psum_scatter(
        mixed_part.astype(jnp.bfloat16), "tp", scatter_dimension=1, tiled=True
    ).astype(jnp.float32)
    residual = (tokens.astype(jnp.float32) + mixed_cols).astype(jnp.bfloat16)
    block_two = gathered_rows(residual).astype(jnp.float32)
    squares_two = jnp.sum(block_two * block_two, axis=1)
    normed_two = (block_two * channel_gain).astype(jnp.bfloat16)
    partial_two = jnp.concatenate(
        [
            jnp.dot(normed_two, ffn_gate, preferred_element_type=jnp.float32),
            jnp.dot(normed_two, ffn_up, preferred_element_type=jnp.float32),
        ],
        axis=1,
    )
    hidden_units = ffn_gate.shape[1]
    summed = every_sum(partial_two, squares_two)
    hidden = (jax.nn.silu(summed[:, :hidden_units]) * summed[:, hidden_units:]).astype(jnp.bfloat16)
    down_part = jnp.dot(hidden, ffn_down, preferred_element_type=jnp.float32)
    down_sums = lax.psum_scatter(
        down_part.astype(jnp.bfloat16), "tp", scatter_dimension=1, tiled=True
    ).astype(jnp.float32)
    layer_output = (residual.astype(jnp.float32) + down_sums).astype(jnp.bfloat16)
    return (layer_output, new_state)


MESH_ID = pl.DeviceIdType.MESH
VMEM_TOTAL = 67043328
CORES = 2


def greet(groups):
    barrier = pltpu.get_barrier_semaphore()
    for axis, peers in groups:
        for peer in peers:
            pl.semaphore_signal(barrier, inc=1, device_id={axis: peer}, device_id_type=MESH_ID)
    pl.semaphore_wait(barrier, sum(len(peers) for _, peers in groups))


def send_all(axis, count, me, source, target, send_sems, recv_sems):
    copies = []
    for step in range(1, count):
        peer = lax.rem(me + step, count)
        copy = pltpu.make_async_remote_copy(
            src_ref=source(peer),
            dst_ref=target(step),
            send_sem=send_sems.at[step - 1],
            recv_sem=recv_sems.at[step - 1],
            device_id={axis: peer},
            device_id_type=MESH_ID,
        )
        copy.start()
        copies.append(copy)
    return copies


def received(copies):
    for copy in copies:
        copy.wait_recv()


def sent(copies):
    for copy in copies:
        copy.wait_send()


def load_all(pairs, sems):
    copies = [pltpu.make_async_copy(src, dst, sems.at[i]) for i, (src, dst) in enumerate(pairs)]
    for copy in copies:
        copy.start()
    return copies


def silu(value):
    return value / (1.0 + jnp.exp(-value))


def square_block(squares):
    head = squares.astype(jnp.bfloat16).astype(jnp.float32)
    rest = squares - head
    lane = lax.broadcasted_iota(jnp.int32, (squares.shape[0], LANES), 1)
    return jnp.where(lane < LANES // 2, head, rest).astype(jnp.bfloat16)


def square_total(block):
    return block[:, :1] + block[:, LANES // 2 : LANES // 2 + 1]


def wide(ref):
    return jnp.concatenate([ref[j] for j in range(ref.shape[0])], axis=1)


def remote(axis, peer, source, target, send_sem, recv_sem):
    return pltpu.make_async_remote_copy(
        src_ref=source, dst_ref=target, send_sem=send_sem, recv_sem=recv_sem,
        device_id={axis: peer}, device_id_type=MESH_ID,
    )


def gather_tp(slots, source, tp, n_tp, send_sems, recv_sems):
    chips = n_tp // CORES
    chip, core = tp // CORES, lax.rem(tp, CORES)
    partner = chip * CORES + 1 - core
    direct = []
    for step in range(1, chips):
        peer = lax.rem(chip + step, chips) * CORES + core
        direct.append(
            remote("tp", peer, source, slots.at[tp], send_sems.at[step], recv_sems.at[step])
        )
    across = [remote("tp", partner, source, slots.at[tp], send_sems.at[0], recv_sems.at[0])]
    for copy in direct + across:
        copy.start()

    def finish():
        for step in range(1, chips):
            direct[step - 1].wait_recv()
            slot = lax.rem(chip - step + chips, chips) * CORES + core
            i = chips - 1 + step
            copy = remote(
                "tp", partner, slots.at[slot], slots.at[slot], send_sems.at[i], recv_sems.at[i]
            )
            copy.start()
            across.append(copy)
        received(across)
        return direct + across

    return finish


def reduce_tp(lhs, weight, parts, swapped, staged, landed, tp, n_tp, send_sems, recv_sems):
    chips = n_tp // CORES
    chip, core = tp // CORES, lax.rem(tp, CORES)
    partner = chip * CORES + 1 - core
    columns = parts.shape[3]

    def multiply(side):
        starts = [pl.multiple_of((z * CORES + side) * columns, LANES) for z in range(chips)]
        rhs = jnp.concatenate([weight[:, pl.ds(start, columns)] for start in starts], axis=1)
        full = jnp.dot(lhs, rhs, preferred_element_type=jnp.float32).astype(jnp.bfloat16)
        for z in range(chips):
            parts[side, z] = full[:, z * columns : (z + 1) * columns]

    multiply(1 - core)
    swap = remote(
        "tp", partner, parts.at[1 - core], swapped, send_sems.at[0], recv_sems.at[0]
    )
    swap.start()
    multiply(core)
    swap.wait_recv()
    copies = []
    for step in range(1, chips):
        other = lax.rem(chip + step, chips)
        pair = parts[core, other].astype(jnp.float32) + swapped[other].astype(jnp.float32)
        staged[step - 1] = pair.astype(jnp.bfloat16)
        copy = remote(
            "tp", other * CORES + core, staged.at[step - 1], landed.at[step - 1],
            send_sems.at[step], recv_sems.at[step],
        )
        copy.start()
        copies.append(copy)
    total = parts[core, chip].astype(jnp.float32) + swapped[chip].astype(jnp.float32)
    for step in range(1, chips):
        copies[step - 1].wait_recv()
        total += landed[step - 1].astype(jnp.float32)
    return total, copies + [swap]


def total_of(own, landed):
    total = own.astype(jnp.float32)
    for step in range(landed.shape[0]):
        total += landed[step].astype(jnp.float32)
    return total


def layer_kernel(
    n_kv, n_tp, features,
    tokens_hbm, lengths_hbm, freq_hbm, gain_hbm, gain_two_hbm, state_hbm,
    wq_hbm, wk_hbm, wv_hbm, wg_hbm, wo_hbm, fg_hbm, fu_hbm, fd_hbm,
    out, state_out,
    state, lengths, freq, gain, gain_two, wq, wk, wv, wg, wo, fg, fu, fd,
    gathered, out_a, out_b, in_a, in_b, qk, value, retained, merged,
    parts_x, swapped_x, staged_x, landed_x, own, gathered_two,
    gate_out, up_out, gate_in, up_in, hidden, parts_d, swapped_d, staged_d, landed_d,
    load_sems, store_sem, gs, gr, as_, ar, bs, br, ms, mr, xs, xr, cs, cr, es, er, fs, fr, hs, hr, ds_, dr,
):
    kv, tp = lax.axis_index("kv"), lax.axis_index("tp")
    chips = n_tp // CORES
    chip, core = tp // CORES, lax.rem(tp, CORES)
    pairs = [
        (tokens_hbm, gathered.at[tp]), (lengths_hbm, lengths), (freq_hbm, freq), (gain_hbm, gain),
        (wq_hbm, wq), (wk_hbm, wk), (wv_hbm, wv), (wg_hbm, wg), (state_hbm, state),
        (gain_two_hbm, gain_two), (wo_hbm, wo), (fg_hbm, fg), (fu_hbm, fu), (fd_hbm, fd),
    ]
    loads = load_all(pairs, load_sems)
    along = [lax.rem(chip + step, chips) * CORES + core for step in range(1, chips)]
    greet([
        ("tp", along + [chip * CORES + 1 - core]),
        ("kv", [lax.rem(kv + step, n_kv) for step in range(1, n_kv)]),
    ])
    loads[0].wait()
    finish_g = gather_tp(gathered, gathered.at[tp], tp, n_tp, gs, gr)
    for i in (1, 2, 3):
        loads[i].wait()
    rows = out_a.shape[1]
    row = lax.broadcasted_iota(jnp.int32, (rows, rows), 0)
    col = lax.broadcasted_iota(jnp.int32, (rows, rows), 1)
    spread = jnp.where(row == col, lengths[...].astype(jnp.float32), 0.0)
    angles = jnp.sum(spread, axis=1, keepdims=True) * freq[...]
    cosine, sine = jnp.cos(angles), jnp.sin(angles)
    lane = lax.broadcasted_iota(jnp.int32, angles.shape, 1)
    sine = jnp.where(lane < QK // 2, -sine, sine)
    started = finish_g()

    def normalise(slots, gains):
        x = wide(slots).astype(jnp.float32)
        squares = jnp.sum(x * x, axis=1, keepdims=True)
        return (x * gains[...]).astype(jnp.bfloat16), square_block(squares).reshape(n_kv, rows, LANES)

    def project(lhs, weight):
        full = jnp.dot(lhs, weight[...], preferred_element_type=jnp.float32)
        return full.astype(jnp.bfloat16).reshape(n_kv, rows, full.shape[1])

    normed, squares = normalise(gathered, gain)
    q_width, v_width = wq.shape[1], wv.shape[1]
    heads = q_width // QK
    width = v_width // heads
    out_a[:, :, 2 * q_width :] = squares
    loads[4].wait()
    out_a[:, :, :q_width] = project(normed, wq)
    loads[5].wait()
    out_a[:, :, q_width : 2 * q_width] = project(normed, wk)
    first = send_all("kv", n_kv, kv, lambda p: out_a.at[p], lambda s: in_a.at[s - 1], as_, ar)
    loads[6].wait()
    out_b[:, :, :v_width] = project(normed, wv)
    loads[7].wait()
    out_b[:, :, v_width:] = project(normed, wg)
    second = send_all("kv", n_kv, kv, lambda p: out_b.at[p], lambda s: in_b.at[s - 1], bs, br)
    loads[8].wait()
    received(first)
    total = total_of(out_a[kv], in_a)
    scale = lax.rsqrt(square_total(total[:, 2 * q_width :]) / features + 1e-06)
    total = total * scale
    blocks = []
    for base, factor in ((0, 1.0), (q_width, QK ** (-0.5))):
        for head in range(heads):
            part = total[:, base + head * QK : base + (head + 1) * QK]
            turned = (part * cosine + pltpu.roll(part, QK // 2, 1) * sine) * factor
            blocks.append(turned.astype(jnp.bfloat16).astype(jnp.float32))
    qk[...] = jnp.concatenate(blocks, axis=0).T
    block = 4

    def turned_to(start):
        return pltpu.roll(qk[...], lax.rem(LANES - start, LANES), 1)

    def query_step(i, carry):
        start = i * block
        turned = turned_to(start)
        for s in range(block):
            for head in range(heads):
                query = turned[:, head * rows + s : head * rows + s + 1]
                retained[pl.ds(start + s, 1), head * width : (head + 1) * width] = jnp.sum(
                    query * state[start + s, head], axis=0, keepdims=True
                )
        return carry

    lax.fori_loop(0, rows // block, query_step, 0)
    decays = []
    for head in range(heads):
        number = jnp.full((1, width), tp * heads + head, jnp.int32).astype(jnp.float32)
        decays.append(1.0 - jnp.exp2(-5.0 - 10.0 * number / (heads * n_tp - 1)))
    received(second)
    total = total_of(out_b[kv], in_b) * scale
    value[...] = total[:, :v_width].astype(jnp.bfloat16).astype(jnp.float32)
    pieces = []
    for head in range(heads):
        overlap = jnp.sum(blocks[head] * blocks[heads + head], axis=1, keepdims=True)
        span = slice(head * width, (head + 1) * width)
        piece = decays[head] * retained[:, span] + overlap * value[:, span]
        pieces.append(piece * lax.rsqrt(jnp.mean(piece * piece, axis=1, keepdims=True) + 1e-06))
    merged[kv] = (jnp.concatenate(pieces, axis=1) * silu(total[:, v_width:])).astype(jnp.bfloat16)
    copies_m = send_all("kv", n_kv, kv, lambda p: merged.at[kv], lambda s: merged.at[kv], ms, mr)

    def update_step(i, carry):
        start = i * block
        turned = turned_to(start)
        for s in range(block):
            for head in range(heads):
                lane = (heads + head) * rows + s
                outer = turned[:, lane : lane + 1] * value[pl.ds(start + s, 1), head * width : (head + 1) * width]
                state[start + s, head] = decays[head] * state[start + s, head] + outer
        return carry

    lax.fori_loop(0, rows // block, update_step, 0)
    loads[10].wait()
    received(copies_m)
    store = pltpu.make_async_copy(state, state_out, store_sem)
    store.start()
    batch = n_kv * rows
    total, copies_x = reduce_tp(
        merged[...].reshape(batch, v_width), wo, parts_x, swapped_x, staged_x, landed_x, tp, n_tp, xs, xr
    )
    residual = (tokens_of(gathered, tp) + total).astype(jnp.bfloat16)
    own[...] = residual
    gathered_two[tp] = residual
    finish_c = gather_tp(gathered_two, own, tp, n_tp, cs, cr)
    loads[9].wait()
    loads[11].wait()
    copies_c = finish_c()
    normed, squares = normalise(gathered_two, gain_two)
    units = fg.shape[1]
    gate_out[:, :, units:] = squares
    gate_out[:, :, :units] = project(normed, fg)
    copies_e = send_all("kv", n_kv, kv, lambda p: gate_out.at[p], lambda s: gate_in.at[s - 1], es, er)
    loads[12].wait()
    up_out[...] = project(normed, fu)
    copies_f = send_all("kv", n_kv, kv, lambda p: up_out.at[p], lambda s: up_in.at[s - 1], fs, fr)
    received(copies_e)
    total = total_of(gate_out[kv], gate_in)
    scale = lax.rsqrt(square_total(total[:, units:]) / features + 1e-06)
    activated = silu(total[:, :units] * scale)
    received(copies_f)
    hidden[kv] = (activated * (total_of(up_out[kv], up_in) * scale)).astype(jnp.bfloat16)
    copies_h = send_all("kv", n_kv, kv, lambda p: hidden.at[kv], lambda s: hidden.at[kv], hs, hr)
    loads[13].wait()
    received(copies_h)
    total, copies_d = reduce_tp(
        hidden[...].reshape(batch, units), fd, parts_d, swapped_d, staged_d, landed_d, tp, n_tp, ds_, dr
    )
    out[...] = (own[...].astype(jnp.float32) + total).astype(jnp.bfloat16)
    for copies in (started, first, second, copies_m, copies_x, copies_c, copies_e, copies_f, copies_h, copies_d):
        sent(copies)
    store.wait()


def finish_kernel(state, out, state_to, out_to, slots, small, load_sems, store_sems):
    chunks, size = slots.shape[0], slots.shape[1]
    pairs, targets = [(out, small)], [(small, out_to)]
    for i in range(chunks):
        pairs.append((state.at[pl.ds(i * size, size)], slots.at[i]))
        targets.append((slots.at[i], state_to.at[pl.ds(i * size, size)]))
    loads = load_all(pairs, load_sems)
    stores = []
    for i, (source, target) in enumerate(targets):
        loads[i].wait()
        copy = pltpu.make_async_copy(source, target, store_sems.at[i])
        copy.start()
        stores.append(copy)
    for copy in stores:
        copy.wait()


def tokens_of(slots, tp):
    return slots[tp].astype(jnp.float32)


def fused_on_device(n_kv, n_tp, *arrays):
    (
        tokens, lengths, state, mixer_gain, wq, wk, wv, wg, wo, channel_gain, fg, fu, fd,
    ) = arrays
    batch, columns = tokens.shape
    rows = state.shape[0]
    depth, q_width = wq.shape
    v_width, units = wv.shape[1], fg.shape[1]
    bf16, f32 = jnp.bfloat16, jnp.float32
    vmem = pl.BlockSpec(memory_space=pltpu.VMEM)
    hbm = pl.BlockSpec(memory_space=pltpu.HBM)
    dma = pltpu.SemaphoreType.DMA
    tp_sems, kv_sems = [dma((n_tp - 1,))] * 2, [dma((n_kv - 1,))] * 2
    chips = n_tp // CORES
    chip_sems = [dma((chips,))] * 2
    index = np.arange(QK) % (QK // 2)
    freq = jnp.asarray((10000.0 ** (-index / (QK // 2))).astype(np.float32))[None, :]
    a_width, b_width = 2 * q_width + LANES, 2 * v_width
    reduce_scratch = [
        pltpu.VMEM((CORES, chips, batch, columns), bf16),
        pltpu.VMEM((chips, batch, columns), bf16),
        pltpu.VMEM((chips - 1, batch, columns), bf16),
        pltpu.VMEM((chips - 1, batch, columns), bf16),
    ]
    out, new_state = pl.pallas_call(
        functools.partial(layer_kernel, n_kv, n_tp, depth * n_kv),
        out_shape=(
            jax.ShapeDtypeStruct(tokens.shape, bf16),
            jax.ShapeDtypeStruct(state.shape, f32),
        ),
        in_specs=[hbm] * 14,
        out_specs=(vmem, hbm),
        scratch_shapes=[
            pltpu.VMEM(state.shape, f32),
            pltpu.VMEM((1, rows), jnp.int32),
            pltpu.VMEM((1, QK), f32),
            pltpu.VMEM((1, depth), f32),
            pltpu.VMEM((1, depth), f32),
        ]
        + [pltpu.VMEM(w.shape, bf16) for w in (wq, wk, wv, wg, wo, fg, fu, fd)]
        + [
            pltpu.VMEM((n_tp, batch, columns), bf16),
            pltpu.VMEM((n_kv, rows, a_width), bf16),
            pltpu.VMEM((n_kv, rows, b_width), bf16),
            pltpu.VMEM((n_kv - 1, rows, a_width), bf16),
            pltpu.VMEM((n_kv - 1, rows, b_width), bf16),
            pltpu.VMEM((QK, LANES), f32),
            pltpu.VMEM((rows, v_width), f32),
            pltpu.VMEM((rows, v_width), f32),
            pltpu.VMEM((n_kv, rows, v_width), bf16),
        ]
        + reduce_scratch
        + [
            pltpu.VMEM((batch, columns), bf16),
            pltpu.VMEM((n_tp, batch, columns), bf16),
            pltpu.VMEM((n_kv, rows, units + LANES), bf16),
            pltpu.VMEM((n_kv, rows, units), bf16),
            pltpu.VMEM((n_kv - 1, rows, units + LANES), bf16),
            pltpu.VMEM((n_kv - 1, rows, units), bf16),
            pltpu.VMEM((n_kv, rows, units), bf16),
        ]
        + reduce_scratch
        + [dma((14,)), dma]
        + tp_sems + kv_sems + kv_sems + kv_sems + chip_sems + tp_sems + kv_sems + kv_sems + kv_sems + chip_sems,
        compiler_params=pltpu.CompilerParams(
            collective_id=0, has_side_effects=True, vmem_limit_bytes=VMEM_TOTAL
        ),
        name="layer",
    )(tokens, lengths[None, :], freq, mixer_gain[None, :], channel_gain[None, :], state, wq, wk, wv, wg, wo, fg, fu, fd)
    chunks = 8
    new_state, out = pl.pallas_call(
        finish_kernel,
        out_shape=(
            jax.ShapeDtypeStruct(state.shape, f32),
            jax.ShapeDtypeStruct(tokens.shape, bf16),
        ),
        in_specs=[hbm, hbm],
        out_specs=(hbm, hbm),
        scratch_shapes=[
            pltpu.VMEM((chunks, rows // chunks) + state.shape[1:], f32),
            pltpu.VMEM(tokens.shape, bf16),
            dma((chunks + 1,)),
            dma((chunks + 1,)),
        ],
        compiler_params=pltpu.CompilerParams(vmem_limit_bytes=VMEM_TOTAL),
        name="finish",
    )(new_state, out)
    return out, new_state


def fits(n_kv, n_tp, arrays):
    tokens, state, ffn_gate = arrays[0], arrays[2], arrays[10]
    rows, heads = state.shape[0], state.shape[1]
    return (
        tokens.shape[1] % LANES == 0
        and n_tp % CORES == 0
        and n_tp > CORES
        and n_kv > 1
        and 4 * state.size < VMEM_TOTAL // 4
        and ffn_gate.shape[1] % LANES == 0
        and rows % 16 == 0
        and 2 * heads * rows == LANES
        and state.shape[2] == QK == LANES
        and state.shape[3] % LANES == 0
    )


def per_device(n_kv, n_tp, *arrays):
    if fits(n_kv, n_tp, arrays):
        return fused_on_device(n_kv, n_tp, *arrays)
    return on_device(*arrays)


def solution(mesh):
    in_specs = (
        P(None, ("kv", "tp")),
        P("kv"),
        P("kv", "tp", None, None),
        P("kv"),
        P("kv", "tp"),
        P("kv", "tp"),
        P("kv", "tp"),
        P("kv", "tp"),
        P("tp", "kv"),
        P("kv"),
        P("kv", "tp"),
        P("kv", "tp"),
        P("tp", "kv"),
    )
    out_specs = (P(None, ("kv", "tp")), P("kv", "tp", None, None))
    return jax.shard_map(
        functools.partial(per_device, mesh.shape["kv"], mesh.shape["tp"]),
        mesh=mesh, in_specs=in_specs, out_specs=out_specs, check_vma=False
    )
```
